32 devices in a mesh: sp: 4 (over z), fs: 4 (over y, x), tp: 2 (over core).
Axes of the slice: x: 2, y: 2, z: 4, core: 2. Of those that a mesh axis runs over, the one named last changes fastest.
Arguments:
- tokens: bfloat16 [4, 2048, 2048], P('fs', 'sp'), may hold values from -6 to 6
- input_gain: float32 [2048], replicated, may hold values from 0.1 to 1.9
- weight_gate: bfloat16 [2048, 2048], P('sp', 'tp'), may hold values from -0.125 to 0.125
- weight_input: bfloat16 [2048, 2048], P('sp', 'tp'), may hold values from -0.125 to 0.125
- weight_write: bfloat16 [2048, 1024], P('sp', 'tp'), may hold values from -0.125 to 0.125
- weight_read: bfloat16 [2048, 1024], P('sp', 'tp'), may hold values from -0.125 to 0.125
- weight_step: bfloat16 [2048, 32], P('sp', 'tp'), may hold values from -0.125 to 0.125
- weight_value: bfloat16 [2048, 2048], P('sp', 'tp'), may hold values from -0.125 to 0.125
- weight_sigmoid: bfloat16 [2048, 2048], P('sp', 'tp'), may hold values from -0.125 to 0.125
- filter_input: bfloat16 [4, 2048], P(None, 'tp'), may hold values from -3 to 3
- filter_write: bfloat16 [4, 1024], P(None, 'tp'), may hold values from -3 to 3
- filter_read: bfloat16 [4, 1024], P(None, 'tp'), may hold values from -3 to 3
- step_bias: float32 [32], P('tp'), may hold values from -4.5 to -3.5
- rate_log: float32 [32], P('tp'), as said below
- skip_gain: float32 [32], P('tp'), may hold values from 0.1 to 1.9
- output_gain: float32 [2048], P('tp'), may hold values from 0.1 to 1.9
- opening_state: float32 [4, 32, 64, 128], P('fs', 'tp'), may hold values from -12 to 12
- decay_shift: float32 [4, 32, 2048], P('fs', 'tp', 'sp'), may hold values from -3 to 0, as said below
- depth_filter: bfloat16 [31, 2048], P(None, 'tp'), may hold values from -40 to 40
- channel_gain: float32 [2048], P('tp'), may hold values from 0.1 to 1.9
- unproject_state: bfloat16 [2048, 2048], P('tp', 'sp'), may hold values from -0.09375 to 0.09375
- unproject_filter: bfloat16 [2048, 2048], P('tp', 'sp'), may hold values from -0.09375 to 0.09375
Outputs:
- mixed: bfloat16 [4, 2048, 2048], P('fs', ('sp', 'tp'))
The draws below stay inside these ranges and needn't reach their ends.
Inputs may be any that keep to these rules, and one draw needn't show every extreme that they name: `rate_log`: logarithms of the heads' decay rates. `decay_shift`: Non-positive.
All inputs are finite; a program needn't handle non-finite values.
Results may differ from the reference program's by a relative error of at most 0.018.
Values may be sent and summed in bfloat16 or wider, within the bound.
A program may use at most 128 MiB of HBM per device.

```python
import math
from functools import partial
import jax
import jax.numpy as jnp
from jax import lax

D = 2048
HEADS = 32
HEAD_DIM = 64
GROUPS = 8
STATE = 128
CM = 2048
SSD_CONV = 4
CONV_SPAN = 31
BLOCK = 128
TOK_DEV = 512
SSD_WIDTH = 2048
SEQS = 4
LENGTH = 2048
N_TP = 2


def draw_rate_log(key, part):
    pick_key, slow_key, fast_key = jax.random.split(jax.random.fold_in(key, 11), 3)
    slow_share = 0.5
    slow_heads = jax.random.uniform(pick_key, (HEADS,), jnp.float32) < slow_share
    slow_rate = jnp.exp(jax.random.uniform(slow_key, (HEADS,), jnp.float32, math.log(10.0), math.log(33.0))) / LENGTH
    fast_rate = jnp.exp(jax.random.uniform(fast_key, (HEADS,), jnp.float32, math.log(0.7), math.log(1.5)))
    return jnp.log(jnp.where(slow_heads, slow_rate, fast_rate)).astype(jnp.float32)


def draw_decay_shift(key, part):
    factor_key, spot_key, depth_key, noise_key = jax.random.split(jax.random.fold_in(key, 23), 4)
    lowest = math.log(0.5)
    factors = jnp.exp(jax.random.uniform(factor_key, (SEQS, LENGTH // TOK_DEV), jnp.float32, lowest, math.log(2.0)))
    background_intensity = -(0.3 / LENGTH) * jnp.repeat(factors, TOK_DEV, axis=1)
    stochastic_perturbation = jax.random.uniform(noise_key, (SEQS, HEADS, LENGTH), jnp.float32, 0.5, 1.5)
    selected_locations = jax.random.randint(spot_key, (SEQS, 4), 0, LENGTH)
    kernel_channel_counts = jnp.log(jax.random.uniform(depth_key, (SEQS, 4), jnp.float32, 0.5, 0.8))
    sequence_indices = jnp.arange(LENGTH, dtype=jnp.int32)
    spike_occurrences = jnp.sum(jnp.where(sequence_indices[None, None, :] == selected_locations[:, :, None], kernel_channel_counts[:, :, None], 0.0), axis=1)
    return (background_intensity[:, None, :] * stochastic_perturbation + spike_occurrences[:, None, :]).astype(jnp.float32)


def draw_depth_filter(key, part):
    value_key, scale_key = jax.random.split(jax.random.fold_in(key, 37), 2)
    top_scale = math.log(10.0)
    ramp = jnp.arange(CM, dtype=jnp.float32) / (CM - 1)
    scales = jnp.exp(ramp * top_scale) * jnp.exp(jax.random.uniform(scale_key, (CM,), jnp.float32, 0.0, math.log(1.5)))
    values = jax.random.truncated_normal(value_key, -4.0, 4.0, (CONV_SPAN, CM), jnp.float32)
    return (values * scales[None, :] / math.sqrt(CONV_SPAN)).astype(jnp.bfloat16)


def block_levels(key, extent, cuts, low, largest):
    loudness, own = 1.0, jax.random.fold_in(key, 6)
    for axis_at, parts in cuts:
        steps = jnp.exp(jax.random.uniform(jax.random.fold_in(own, axis_at), (parts,), jnp.float32, low / len(cuts), largest / len(cuts)))
        loudness = loudness * jnp.repeat(steps, extent[axis_at] // parts).reshape([-1 if axis == axis_at else 1 for axis in range(len(extent))])
    return loudness


def normal_values(key, dims, scale, most, cuts=(), held_as=jnp.bfloat16):
    gain = block_levels(key, dims, cuts, -0.22, 0.18) if cuts else 1.0
    values = jax.random.normal(key, dims, jnp.float32) * scale * gain
    return jnp.minimum(jnp.maximum(values, -most), most).astype(held_as)


def setup_inputs(seed: int = 0) -> dict:
    streams_of = jax.random.split(jax.random.key(seed), 23)
    return {
        "tokens": normal_values(streams_of[0], (SEQS, LENGTH, D), 1.0, 6.0, ((0, 4), (1, 4))),
        "input_gain": jnp.clip(1.0 + 0.18 * jax.random.normal(streams_of[1], (D,), jnp.float32), 0.1, 1.9),
        "weight_gate": normal_values(streams_of[2], (D, SSD_WIDTH), D ** -0.5, 0.125, ((0, 4), (1, 2))),
        "weight_input": normal_values(streams_of[3], (D, SSD_WIDTH), D ** -0.5, 0.125, ((0, 4), (1, 2))),
        "weight_write": normal_values(streams_of[4], (D, GROUPS * STATE), D ** -0.5, 0.125, ((0, 4), (1, 2))),
        "weight_read": normal_values(streams_of[5], (D, GROUPS * STATE), D ** -0.5, 0.125, ((0, 4), (1, 2))),
        "weight_step": normal_values(streams_of[6], (D, HEADS), D ** -0.5, 0.125, ((0, 4), (1, 2))),
        "weight_value": normal_values(streams_of[7], (D, CM), D ** -0.5, 0.125, ((0, 4), (1, 2))),
        "weight_sigmoid": normal_values(streams_of[8], (D, CM), D ** -0.5, 0.125, ((0, 4), (1, 2))),
        "filter_input": normal_values(streams_of[9], (SSD_CONV, SSD_WIDTH), SSD_CONV ** -0.5, 3.0, ((1, 2),)),
        "filter_write": normal_values(streams_of[10], (SSD_CONV, GROUPS * STATE), SSD_CONV ** -0.5, 3.0, ((1, 2),)),
        "filter_read": normal_values(streams_of[11], (SSD_CONV, GROUPS * STATE), SSD_CONV ** -0.5, 3.0, ((1, 2),)),
        "step_bias": jnp.clip(-4.5 + 1.0 * jax.random.uniform(streams_of[12], (HEADS,), jnp.float32) ** block_levels(streams_of[12], (HEADS,), ((0, 2),), -0.2, 0.2), -4.5, -3.5),
        "rate_log": draw_rate_log(jax.random.fold_in(streams_of[22], 71), 0),
        "skip_gain": jnp.clip(1.0 + 0.18 * jax.random.normal(streams_of[14], (HEADS,), jnp.float32), 0.1, 1.9),
        "output_gain": jnp.clip(1.0 + 0.18 * jax.random.normal(streams_of[15], (SSD_WIDTH,), jnp.float32), 0.1, 1.9),
        "opening_state": normal_values(streams_of[16], (SEQS, HEADS, HEAD_DIM, STATE), 2.0, 12.0, ((0, 4), (1, 2)), jnp.float32),
        "decay_shift": draw_decay_shift(jax.random.fold_in(streams_of[22], 71), 0),
        "depth_filter": draw_depth_filter(jax.random.fold_in(streams_of[22], 71), 0),
        "channel_gain": jnp.clip(1.0 + 0.18 * jax.random.normal(streams_of[19], (CM,), jnp.float32), 0.1, 1.9),
        "unproject_state": normal_values(streams_of[20], (SSD_WIDTH, D), (SSD_WIDTH + CM) ** -0.5, 0.09375, ((0, 2), (1, 4))),
        "unproject_filter": normal_values(streams_of[21], (CM, D), (SSD_WIDTH + CM) ** -0.5, 0.09375, ((0, 2), (1, 4))),
    }


exact_mode = lax.Precision.HIGHEST

def causal_filter(border, values, kernel):
    extended = jnp.concatenate([border, values], axis=0).astype(jnp.float32)
    weights = kernel.astype(jnp.float32)
    row_count = values.shape[0]
    result = jnp.zeros(values.shape, jnp.float32)
    for offset in range(kernel.shape[0]):
        result = result + weights[offset] * extended[offset:offset + row_count]
    return result

def block_step(direct_gain, memory, pieces):
    input_block, write_block, read_block, step_block, log_block = pieces
    head_count = input_block.shape[1]
    per_group = head_count // write_block.shape[1]
    running = jnp.cumsum(log_block, axis=0)
    write_heads = jnp.repeat(write_block, per_group, axis=1)
    read_heads = jnp.repeat(read_block, per_group, axis=1)
    scores = jnp.einsum('lhn,shn->hls', read_heads, write_heads, precision=exact_mode)
    spread = running.T[:, :, None] - running.T[:, None, :]
    row_index = lax.broadcasted_iota(jnp.int32, spread.shape, 1)
    col_index = lax.broadcasted_iota(jnp.int32, spread.shape, 2)
    decays = jnp.exp(jnp.where(row_index >= col_index, spread, -jnp.inf))
    scaled_inputs = input_block * step_block[:, :, None]
    inside = jnp.einsum('hls,shp->lhp', scores * decays, scaled_inputs, precision=exact_mode)
    carried = jnp.exp(running)[:, :, None] * jnp.einsum('lhn,hpn->lhp', read_heads, memory, precision=exact_mode)
    output = inside + carried + direct_gain[None, :, None] * input_block
    to_end = jnp.exp(running[-1][None, :] - running)
    fresh_terms = jnp.einsum('lhp,lhn->hpn', scaled_inputs * to_end[:, :, None], write_heads, precision=exact_mode)
    new_memory = jnp.exp(running[-1])[:, None, None] * memory + fresh_terms
    return (new_memory, output)

def reference(tokens, input_gain, weight_gate, weight_input, weight_write, weight_read, weight_step, weight_value, weight_sigmoid, filter_input, filter_write, filter_read, step_bias, rate_log, skip_gain, output_gain, opening_state, decay_shift, depth_filter, channel_gain, unproject_state, unproject_filter):

    def project(normed, weight):
        return jnp.dot(normed, weight, preferred_element_type=jnp.float32).astype(jnp.bfloat16)

    def one_sequence(packed):
        sequence, start_memory, shift_rows = packed
        source = sequence.astype(jnp.float32)
        normed = (source * lax.rsqrt(lax.optimization_barrier(jnp.mean(source * source, axis=-1, keepdims=True)) + 1e-06) * input_gain).astype(jnp.bfloat16)
        gate_values = project(normed, weight_gate)
        input_values = project(normed, weight_input)
        write_values = project(normed, weight_write)
        read_values = project(normed, weight_read)
        step_values = project(normed, weight_step)
        value_rows = project(normed, weight_value)
        sigmoid_rows = project(normed, weight_sigmoid)
        glu_rows = (value_rows.astype(jnp.float32) * jax.nn.sigmoid(sigmoid_rows.astype(jnp.float32))).astype(jnp.bfloat16)
        short_rim = SSD_CONV - 1
        mixed_input = jax.nn.silu(causal_filter(jnp.zeros((short_rim, SSD_WIDTH), jnp.bfloat16), input_values, filter_input)).astype(jnp.bfloat16)
        mixed_write = jax.nn.silu(causal_filter(jnp.zeros((short_rim, GROUPS * STATE), jnp.bfloat16), write_values, filter_write)).astype(jnp.bfloat16)
        mixed_read = jax.nn.silu(causal_filter(jnp.zeros((short_rim, GROUPS * STATE), jnp.bfloat16), read_values, filter_read)).astype(jnp.bfloat16)
        step_sizes = jax.nn.softplus(step_values.astype(jnp.float32) + step_bias)
        log_rates = -step_sizes * jnp.exp(rate_log) + shift_rows.T
        block_count = LENGTH // BLOCK
        inputs_float = mixed_input.astype(jnp.float32).reshape(block_count, BLOCK, HEADS, HEAD_DIM)
        write_float = mixed_write.astype(jnp.float32).reshape(block_count, BLOCK, GROUPS, STATE)
        read_float = mixed_read.astype(jnp.float32).reshape(block_count, BLOCK, GROUPS, STATE)
        blocked = (inputs_float, write_float, read_float, step_sizes.reshape(block_count, BLOCK, HEADS), log_rates.reshape(block_count, BLOCK, HEADS))
        final_memory, outputs = lax.scan(partial(block_step, skip_gain), start_memory, blocked)
        gated = outputs.reshape(LENGTH, SSD_WIDTH) * jax.nn.silu(gate_values.astype(jnp.float32))
        grouped = gated.reshape(LENGTH, GROUPS, SSD_WIDTH // GROUPS)
        grouped = grouped * lax.rsqrt(lax.optimization_barrier(jnp.mean(grouped * grouped, axis=-1, keepdims=True)) + 1e-06)
        state_out = (grouped.reshape(LENGTH, SSD_WIDTH) * output_gain).astype(jnp.bfloat16)
        filtered = causal_filter(jnp.zeros((CONV_SPAN - 1, CM), jnp.bfloat16), glu_rows, depth_filter)
        mean_value = lax.optimization_barrier(jnp.mean(filtered, axis=-1, keepdims=True))
        mean_square = lax.optimization_barrier(jnp.mean(filtered * filtered, axis=-1, keepdims=True))
        variance = mean_square - mean_value * mean_value
        filter_out = jax.nn.silu((filtered - mean_value) * lax.rsqrt(variance + 1e-05) * channel_gain).astype(jnp.bfloat16)
        state_width = SSD_WIDTH // N_TP
        filter_width = CM // N_TP

        def add_term(total, block_index):
            state_cols = lax.dynamic_slice_in_dim(state_out, block_index * state_width, state_width, 1)
            state_weights = lax.dynamic_slice_in_dim(unproject_state, block_index * state_width, state_width, 0)
            filter_cols = lax.dynamic_slice_in_dim(filter_out, block_index * filter_width, filter_width, 1)
            filter_weights = lax.dynamic_slice_in_dim(unproject_filter, block_index * filter_width, filter_width, 0)
            term = jnp.dot(state_cols, state_weights, preferred_element_type=jnp.float32)
            term = term + jnp.dot(filter_cols, filter_weights, preferred_element_type=jnp.float32)
            rounded = lax.optimization_barrier(term.astype(jnp.bfloat16))
            return (total + rounded.astype(jnp.float32), None)
        total, unused = lax.scan(add_term, jnp.zeros((LENGTH, D), jnp.float32), jnp.arange(N_TP, dtype=jnp.int32))
        return total.astype(jnp.bfloat16)
    return lax.map(one_sequence, (tokens, opening_state, decay_shift))
```

```python
import jax
import jax.numpy as jnp
from jax import lax
from jax.experimental import pallas as pl
from jax.experimental.pallas import tpu as pltpu
from jax.sharding import PartitionSpec as P

HEAD_DIM = 64
STATE = 128
CM = 2048
BLOCK = 128


def passed_along(array, axis, by):
    length = lax.axis_size(axis)
    pairs = [(i, i + by) for i in range(length) if 0 <= i + by < length]
    return lax.ppermute(array, axis, pairs)


def causal_filter(border, values, kernel):
    extended = jnp.concatenate([border, values], axis=0).astype(jnp.float32)
    weights = kernel.astype(jnp.float32)
    row_count = values.shape[0]
    result = jnp.zeros(values.shape, jnp.float32)
    for offset in range(kernel.shape[0]):
        result = result + weights[offset] * extended[offset : offset + row_count]
    return result


def gathered(pieces):
    share = lax.axis_size("fs")
    cut = []
    for piece in pieces:
        rows = piece.shape[0] // share
        cut.append(lax.dynamic_slice_in_dim(piece, lax.axis_index("fs") * rows, rows, 0))
    joined = cut[0] if len(cut) == 1 else jnp.concatenate(cut, axis=1)
    return lax.all_gather(joined, ("sp", "fs"), axis=0, tiled=True)


def over_lanes(columns, width):
    rows, count = columns.shape
    lane = lax.broadcasted_iota(jnp.int32, (rows, width), 1) // HEAD_DIM
    result = jnp.broadcast_to(columns[:, 0:1], (rows, width))
    for head in range(1, count):
        result = jnp.where(lane == head, columns[:, head : head + 1], result)
    return result


def local_kernel(
    x_ref, write_ref, read_ref, col_ref, end_ref, row_ref, step_ref, y_ref, state_ref
):
    rows, width = x_ref.shape
    heads = col_ref.shape[2]
    state = jnp.zeros((STATE, width), jnp.float32)
    row_at = lax.broadcasted_iota(jnp.int32, (BLOCK, BLOCK), 0)
    col_at = lax.broadcasted_iota(jnp.int32, (BLOCK, BLOCK), 1)
    lane = lax.broadcasted_iota(jnp.int32, (BLOCK, width), 1) // HEAD_DIM
    for block in range(rows // BLOCK):
        at = pl.ds(block * BLOCK, BLOCK)
        x, write, read = x_ref[at, :], write_ref[at, :], read_ref[at, :]
        columns = col_ref[0, at, :]
        scores = lax.dot_general(
            read, write, (((1,), (1,)), ((), ())), preferred_element_type=jnp.float32
        )
        weights, inputs = [], []
        for head in range(heads):
            spread = columns[:, head : head + 1] - row_ref[0, head : head + 1, at]
            decay = jnp.exp(jnp.where(row_at >= col_at, spread, -jnp.inf))
            weights.append((scores * decay * step_ref[0, head : head + 1, at]).astype(jnp.bfloat16))
            inputs.append(jnp.where(lane == head, x, jnp.zeros_like(x)))
        inside = jnp.dot(
            jnp.concatenate(weights, axis=1),
            jnp.concatenate(inputs, axis=0),
            preferred_element_type=jnp.float32,
        )
        grown = over_lanes(jnp.exp(columns), width)
        if block:
            inside = inside + grown * jnp.dot(
                read, state.astype(jnp.bfloat16), preferred_element_type=jnp.float32
            )
        y_ref[at, :] = inside
        scaled = (x.astype(jnp.float32) * over_lanes(end_ref[0, at, :], width)).astype(jnp.bfloat16)
        fresh = lax.dot_general(
            write, scaled, (((0,), (0,)), ((), ())), preferred_element_type=jnp.float32
        )
        state = state * grown[BLOCK - 1 :, :] + fresh
    state_ref[...] = state


def finish_kernel(
    y_ref, x_ref, read_ref, gate_ref, enter_ref, col_ref, skip_ref, gain_ref, out_ref
):
    rows, width = x_ref.shape
    entering = enter_ref[...].astype(jnp.bfloat16)
    for block in range(rows // BLOCK):
        at = pl.ds(block * BLOCK, BLOCK)
        carried = jnp.dot(read_ref[at, :], entering, preferred_element_type=jnp.float32)
        total = y_ref[at, :] + over_lanes(col_ref[0, at, :], width) * carried
        total = total + skip_ref[...] * x_ref[at, :].astype(jnp.float32)
        gate = gate_ref[at, :].astype(jnp.float32)
        gated = total * (gate * jax.nn.sigmoid(gate))
        size = jnp.mean(gated * gated, axis=1, keepdims=True)
        out_ref[at, :] = (gated * lax.rsqrt(size + 1e-06) * gain_ref[...]).astype(jnp.bfloat16)


def per_device(
    tokens,
    input_gain,
    weight_gate,
    weight_input,
    weight_write,
    weight_read,
    weight_step,
    weight_value,
    weight_sigmoid,
    filter_input,
    filter_write,
    filter_read,
    step_bias,
    rate_log,
    skip_gain,
    output_gain,
    opening_state,
    decay_shift,
    depth_filter,
    channel_gain,
    unproject_state,
    unproject_filter,
):
    row_count = tokens.shape[1]
    length = lax.axis_size("sp")
    head_count = rate_log.shape[0]
    width = weight_input.shape[1]
    group_count = weight_write.shape[1] // STATE
    per_group = head_count // group_count
    group_width = per_group * HEAD_DIM
    source = tokens[0].astype(jnp.float32)
    normed = (
        source * lax.rsqrt(jnp.mean(source * source, axis=-1, keepdims=True) + 1e-06) * input_gain
    ).astype(jnp.bfloat16)

    def project(weight):
        return jnp.dot(normed, weight, preferred_element_type=jnp.float32).astype(jnp.bfloat16)

    mixer_rows = project(gathered((weight_input, weight_write, weight_read, weight_step)))
    glu_pair = project(gathered((weight_value, weight_sigmoid)))
    gate_values = project(gathered((weight_gate,)))
    mixer_width = width + 2 * group_count * STATE
    step_values = mixer_rows[:, mixer_width:]
    mixer_rows = mixer_rows[:, :mixer_width]
    short_rim = filter_input.shape[0] - 1
    long_rim = depth_filter.shape[0] - 1
    mixed = jax.nn.silu(
        causal_filter(
            passed_along(mixer_rows[row_count - short_rim :], "sp", 1),
            mixer_rows,
            jnp.concatenate([filter_input, filter_write, filter_read], axis=1),
        )
    ).astype(jnp.bfloat16)
    step_sizes = jax.nn.softplus(step_values.astype(jnp.float32) + step_bias)
    log_rates = -step_sizes * jnp.exp(rate_log) + decay_shift[0].T
    block_count = row_count // BLOCK
    blocked = jnp.cumsum(log_rates.reshape(block_count, BLOCK, head_count), axis=1)
    block_ends = blocked[:, -1]
    before = jnp.cumsum(block_ends, axis=0) - block_ends
    total_decay = before[-1] + block_ends[-1]
    to_end = jnp.exp(block_ends[:, None] - blocked).reshape(row_count, head_count) * step_sizes
    leading = jnp.exp(blocked + before[:, None]).reshape(row_count, head_count)
    blocked = blocked.reshape(row_count, head_count)

    def as_columns(array):
        return array.reshape(row_count, group_count, per_group).transpose(1, 0, 2)

    def as_rows(array):
        return array.T.reshape(group_count, per_group, row_count)

    wide = pl.BlockSpec((row_count, group_width), lambda g: (0, g))
    write_at, read_at = (width // STATE, width // STATE + group_count)
    write_spec = pl.BlockSpec((row_count, STATE), lambda g: (0, write_at + g))
    read_spec = pl.BlockSpec((row_count, STATE), lambda g: (0, read_at + g))
    column_spec = pl.BlockSpec((1, row_count, per_group), lambda g: (g, 0, 0))
    row_spec = pl.BlockSpec((1, per_group, row_count), lambda g: (g, 0, 0))
    state_spec = pl.BlockSpec((STATE, group_width), lambda g: (0, g))
    line_spec = pl.BlockSpec((1, group_width), lambda g: (0, g))
    local_rows, local_state = pl.pallas_call(
        local_kernel,
        grid=(group_count,),
        in_specs=[wide, write_spec, read_spec, column_spec, column_spec, row_spec, row_spec],
        out_specs=[wide, state_spec],
        out_shape=[
            jax.ShapeDtypeStruct((row_count, width), jnp.float32),
            jax.ShapeDtypeStruct((STATE, width), jnp.float32),
        ],
        cost_estimate=pl.CostEstimate(
            flops=8 * row_count * width * BLOCK, bytes_accessed=8 * row_count * width, transcendentals=0
        ),
    )(
        mixed,
        mixed,
        mixed,
        as_columns(blocked),
        as_columns(to_end),
        as_rows(blocked),
        as_rows(step_sizes),
    )
    decay_line = jnp.repeat(total_decay, HEAD_DIM)[None]
    decay_high = decay_line.astype(jnp.bfloat16)
    decay_low = (decay_line - decay_high.astype(jnp.float32)).astype(jnp.bfloat16)
    payload = jnp.concatenate(
        [
            local_state.astype(jnp.bfloat16),
            decay_high,
            decay_low,
            jnp.zeros((14, width), jnp.bfloat16),
        ],
        axis=0,
    )
    entering, reach = (jnp.zeros((STATE, width), jnp.float32), jnp.zeros((1, width), jnp.float32))
    for distance in range(1, length):
        earlier = passed_along(payload, "sp", distance).astype(jnp.float32)
        entering = entering + jnp.exp(reach) * earlier[:STATE]
        reach = reach + earlier[STATE : STATE + 1] + earlier[STATE + 1 : STATE + 2]
    opening = opening_state[0].reshape(width, STATE).T
    entering = entering + jnp.exp(reach) * opening
    state_out = pl.pallas_call(
        finish_kernel,
        grid=(group_count,),
        in_specs=[wide, wide, read_spec, wide, state_spec, column_spec, line_spec, line_spec],
        out_specs=wide,
        out_shape=jax.ShapeDtypeStruct((row_count, width), jnp.bfloat16),
        cost_estimate=pl.CostEstimate(
            flops=2 * row_count * width * STATE, bytes_accessed=10 * row_count * width, transcendentals=0
        ),
    )(
        local_rows,
        mixed,
        mixed,
        gate_values,
        entering,
        as_columns(leading),
        jnp.repeat(skip_gain, HEAD_DIM)[None],
        output_gain[None],
    )
    channels = weight_value.shape[1]
    glu_rows = (
        glu_pair[:, :channels].astype(jnp.float32)
        * jax.nn.sigmoid(glu_pair[:, channels:].astype(jnp.float32))
    ).astype(jnp.bfloat16)
    filtered = causal_filter(
        passed_along(glu_rows[row_count - long_rim :], "sp", 1), glu_rows, depth_filter
    )
    channel_sums = lax.psum((jnp.sum(filtered, axis=1), jnp.sum(filtered * filtered, axis=1)), "tp")
    mean_value = channel_sums[0] / CM
    mean_square = channel_sums[1] / CM
    variance = mean_square - mean_value * mean_value
    normal_rows = (
        (filtered - mean_value[:, None]) * lax.rsqrt(variance + 1e-05)[:, None] * channel_gain
    )
    filter_out = jax.nn.silu(normal_rows).astype(jnp.bfloat16)
    share = lax.axis_size("fs")
    piece_rows = unproject_state.shape[0] // share
    first = lax.axis_index("fs") * piece_rows
    piece = jnp.concatenate(
        [
            lax.dynamic_slice_in_dim(unproject_state, first, piece_rows, 0),
            lax.dynamic_slice_in_dim(unproject_filter, first, piece_rows, 0),
        ],
        axis=0,
    )
    output_maps = lax.all_gather(piece, ("sp", "fs"), axis=0, tiled=True)
    output_maps = output_maps.reshape(length, share * 2 * piece_rows, piece.shape[1])
    joined = jnp.concatenate(
        [
            part[:, i * piece_rows : (i + 1) * piece_rows]
            for i in range(share)
            for part in (state_out, filter_out)
        ],
        axis=1,
    )
    partial_rows = jnp.concatenate(
        [
            jnp.dot(joined, output_maps[i], preferred_element_type=jnp.float32).astype(jnp.bfloat16)
            for i in range(length)
        ],
        axis=1,
    )
    summed = lax.psum_scatter(partial_rows, "tp", scatter_dimension=0, tiled=True)
    return summed[None]


def solution(mesh):
    in_specs = (
        P("fs", "sp", None),
        P(),
        P("sp", "tp"),
        P("sp", "tp"),
        P("sp", "tp"),
        P("sp", "tp"),
        P("sp", "tp"),
        P("sp", "tp"),
        P("sp", "tp"),
        P(None, "tp"),
        P(None, "tp"),
        P(None, "tp"),
        P("tp"),
        P("tp"),
        P("tp"),
        P("tp"),
        P("fs", "tp", None, None),
        P("fs", "tp", "sp"),
        P(None, "tp"),
        P("tp"),
        P("tp", "sp"),
        P("tp", "sp"),
    )
    out_specs = P("fs", ("sp", "tp"), None)
    return jax.shard_map(
        per_device, mesh=mesh, in_specs=in_specs, out_specs=out_specs, check_vma=False
    )
```

```python
from functools import partial

import jax
import jax.numpy as jnp
from jax import lax
from jax.experimental import pallas as pl
from jax.experimental.pallas import tpu as pltpu
from jax.sharding import PartitionSpec as P

HEAD_DIM = 64
STATE = 128
CM = 2048
BLOCK = 128


def passed_along(array, axis, by):
    length = lax.axis_size(axis)
    pairs = [(i, i + by) for i in range(length) if 0 <= i + by < length]
    return lax.ppermute(array, axis, pairs)


def causal_filter(border, values, kernel):
    extended = jnp.concatenate([border, values], axis=0).astype(jnp.float32)
    weights = kernel.astype(jnp.float32)
    row_count = values.shape[0]
    result = jnp.zeros(values.shape, jnp.float32)
    for offset in range(kernel.shape[0]):
        result = result + weights[offset] * extended[offset : offset + row_count]
    return result


def gathered(pieces):
    share = lax.axis_size("fs")
    cut = []
    for piece in pieces:
        rows = piece.shape[0] // share
        cut.append(lax.dynamic_slice_in_dim(piece, lax.axis_index("fs") * rows, rows, 0))
    joined = cut[0] if len(cut) == 1 else jnp.concatenate(cut, axis=1)
    return lax.all_gather(joined, ("sp", "fs"), axis=0, tiled=True)


def spread_kernel(
    cuts, shard_ref, out_ref, z_send, z_recv, x_send, x_recv, y_send, y_recv,
    u_send, u_recv, v_send, v_recv, own_sem,
):
    length, share = lax.axis_size("sp"), lax.axis_size("fs")
    here, member, side = lax.axis_index("sp"), lax.axis_index("fs"), lax.axis_index("tp")
    rows = shard_ref.shape[0]
    part = rows // share
    half = part // 2
    beside = member + 1 - 2 * lax.rem(member, 2)
    across = lax.rem(member + 2, share)
    corner = lax.rem(beside + 2, share)
    partners = [(lax.rem(here + k, length), member, side) for k in range(1, length)]
    partners += [(here, beside, side), (here, across, side)]
    barrier = pltpu.get_barrier_semaphore()
    for partner in partners:
        pl.semaphore_signal(
            barrier, inc=1, device_id=partner, device_id_type=pl.DeviceIdType.MESH
        )
    pl.semaphore_wait(barrier, len(partners))

    def place(start, size, cut):
        return out_ref.at[pl.ds(pl.multiple_of(start, 16), size), pl.ds(*cut)]

    def move(source, target, send, recv, device):
        return pltpu.make_async_remote_copy(
            src_ref=source, dst_ref=target, send_sem=send, recv_sem=recv,
            device_id=device, device_id_type=pl.DeviceIdType.MESH,
        )

    items = [(c, k) for c in range(len(cuts)) for k in range(1, length)]
    started = []
    for c, k in items:
        source = shard_ref.at[pl.ds(pl.multiple_of(member * part, 16), part), pl.ds(*cuts[c])]
        copy = move(
            source,
            place(here * rows + member * part, part, cuts[c]),
            z_send.at[c, k],
            z_recv.at[c, k],
            partners[k - 1],
        )
        copy.start()
        started.append(copy)
    own = pltpu.make_async_copy(
        shard_ref, out_ref.at[pl.ds(pl.multiple_of(here * rows, 16), rows), :], own_sem
    )
    own.start()

    def first_stage(c, k):
        begin = lax.rem(here + length - k, length) * rows
        spot = place(begin + member * part, part, cuts[c])
        move(spot, spot, z_send.at[c, k], z_recv.at[c, k], partners[k - 1]).wait_recv()
        for send, recv, device in ((x_send, x_recv, partners[-2]), (y_send, y_recv, partners[-1])):
            copy = move(spot, spot, send.at[c, k], recv.at[c, k], device)
            copy.start()
            started.append(copy)

    def second_stage(c, k):
        begin = lax.rem(here + length - k, length) * rows
        spot = place(begin + beside * part, part, cuts[c])
        move(spot, spot, x_send.at[c, k], x_recv.at[c, k], partners[-2]).wait_recv()
        low = place(begin + beside * part, half, cuts[c])
        copy = move(low, low, u_send.at[c, k], u_recv.at[c, k], partners[-1])
        copy.start()
        started.append(copy)
        spot = place(begin + across * part, part, cuts[c])
        move(spot, spot, y_send.at[c, k], y_recv.at[c, k], partners[-1]).wait_recv()
        high = place(begin + across * part + half, half, cuts[c])
        copy = move(high, high, v_send.at[c, k], v_recv.at[c, k], partners[-2])
        copy.start()
        started.append(copy)

    for at, (c, k) in enumerate(items):
        first_stage(c, k)
        if at:
            second_stage(*items[at - 1])
    second_stage(*items[-1])
    for c, k in items:
        begin = lax.rem(here + length - k, length) * rows
        low = place(begin + corner * part, half, cuts[c])
        move(low, low, u_send.at[c, k], u_recv.at[c, k], partners[-1]).wait_recv()
        high = place(begin + corner * part + half, half, cuts[c])
        move(high, high, v_send.at[c, k], v_recv.at[c, k], partners[-2]).wait_recv()
    for copy in started:
        copy.wait_send()
    own.wait()


def spread(pieces):
    width = sum(piece.shape[1] for piece in pieces)
    padded = -(-width // 128) * 128
    rows = pieces[0].shape[0]
    if padded > width:
        pieces = pieces + (jnp.zeros((rows, padded - width), pieces[0].dtype),)
    shard = jnp.concatenate(pieces, axis=1)
    length = lax.axis_size("sp")
    edges = [128 * (padded // 128 * i // 3) for i in range(4)]
    cuts = [(edges[i], edges[i + 1] - edges[i]) for i in range(3)]
    return pl.pallas_call(
        partial(spread_kernel, cuts),
        out_shape=jax.ShapeDtypeStruct((length * rows, padded), shard.dtype),
        in_specs=[pl.BlockSpec(memory_space=pl.ANY)],
        out_specs=pl.BlockSpec(memory_space=pl.ANY),
        scratch_shapes=[pltpu.SemaphoreType.DMA((3, length))] * 10 + [pltpu.SemaphoreType.DMA],
        compiler_params=pltpu.CompilerParams(collective_id=0, has_side_effects=True),
        cost_estimate=pl.CostEstimate(
            flops=10**11, bytes_accessed=4 * length * rows * padded, transcendentals=0
        ),
    )(shard)


def over_lanes(columns, width):
    rows, count = columns.shape
    lane = lax.broadcasted_iota(jnp.int32, (rows, width), 1) // HEAD_DIM
    result = jnp.broadcast_to(columns[:, 0:1], (rows, width))
    for head in range(1, count):
        result = jnp.where(lane == head, columns[:, head : head + 1], result)
    return result


def local_kernel(
    x_ref, write_ref, read_ref, col_ref, end_ref, row_ref, step_ref, y_ref, state_ref
):
    rows, width = x_ref.shape
    heads = col_ref.shape[2]
    state = jnp.zeros((STATE, width), jnp.float32)
    row_at = lax.broadcasted_iota(jnp.int32, (BLOCK, BLOCK), 0)
    col_at = lax.broadcasted_iota(jnp.int32, (BLOCK, BLOCK), 1)
    lane = lax.broadcasted_iota(jnp.int32, (BLOCK, width), 1) // HEAD_DIM
    for block in range(rows // BLOCK):
        at = pl.ds(block * BLOCK, BLOCK)
        x, write, read = x_ref[at, :], write_ref[at, :], read_ref[at, :]
        columns = col_ref[0, at, :]
        scores = lax.dot_general(
            read, write, (((1,), (1,)), ((), ())), preferred_element_type=jnp.float32
        )
        weights, inputs = [], []
        for head in range(heads):
            spread = columns[:, head : head + 1] - row_ref[0, head : head + 1, at]
            decay = jnp.exp(jnp.where(row_at >= col_at, spread, -jnp.inf))
            weights.append((scores * decay * step_ref[0, head : head + 1, at]).astype(jnp.bfloat16))
            inputs.append(jnp.where(lane == head, x, jnp.zeros_like(x)))
        inside = jnp.dot(
            jnp.concatenate(weights, axis=1),
            jnp.concatenate(inputs, axis=0),
            preferred_element_type=jnp.float32,
        )
        grown = over_lanes(jnp.exp(columns), width)
        if block:
            inside = inside + grown * jnp.dot(
                read, state.astype(jnp.bfloat16), preferred_element_type=jnp.float32
            )
        y_ref[at, :] = inside
        scaled = (x.astype(jnp.float32) * over_lanes(end_ref[0, at, :], width)).astype(jnp.bfloat16)
        fresh = lax.dot_general(
            write, scaled, (((0,), (0,)), ((), ())), preferred_element_type=jnp.float32
        )
        state = state * grown[BLOCK - 1 :, :] + fresh
    state_ref[...] = state


def finish_kernel(
    y_ref, x_ref, read_ref, gate_ref, enter_ref, col_ref, skip_ref, gain_ref, out_ref
):
    rows, width = x_ref.shape
    entering = enter_ref[...].astype(jnp.bfloat16)
    for block in range(rows // BLOCK):
        at = pl.ds(block * BLOCK, BLOCK)
        carried = jnp.dot(read_ref[at, :], entering, preferred_element_type=jnp.float32)
        total = y_ref[at, :] + over_lanes(col_ref[0, at, :], width) * carried
        total = total + skip_ref[...] * x_ref[at, :].astype(jnp.float32)
        gate = gate_ref[at, :].astype(jnp.float32)
        gated = total * (gate * jax.nn.sigmoid(gate))
        size = jnp.mean(gated * gated, axis=1, keepdims=True)
        out_ref[at, :] = (gated * lax.rsqrt(size + 1e-06) * gain_ref[...]).astype(jnp.bfloat16)


def per_device(
    tokens,
    input_gain,
    weight_gate,
    weight_input,
    weight_write,
    weight_read,
    weight_step,
    weight_value,
    weight_sigmoid,
    filter_input,
    filter_write,
    filter_read,
    step_bias,
    rate_log,
    skip_gain,
    output_gain,
    opening_state,
    decay_shift,
    depth_filter,
    channel_gain,
    unproject_state,
    unproject_filter,
):
    row_count = tokens.shape[1]
    length = lax.axis_size("sp")
    head_count = rate_log.shape[0]
    width = weight_input.shape[1]
    group_count = weight_write.shape[1] // STATE
    per_group = head_count // group_count
    group_width = per_group * HEAD_DIM
    source = tokens[0].astype(jnp.float32)
    normed = (
        source * lax.rsqrt(jnp.mean(source * source, axis=-1, keepdims=True) + 1e-06) * input_gain
    ).astype(jnp.bfloat16)

    def project(weight):
        return jnp.dot(normed, weight, preferred_element_type=jnp.float32).astype(jnp.bfloat16)

    front = project(
        spread(
            (weight_input, weight_write, weight_read, weight_value, weight_sigmoid, weight_step)
        )
    )
    gate_values = project(gathered((weight_gate,)))
    mixer_width = width + 2 * group_count * STATE
    channels = weight_value.shape[1]
    mixer_rows = front[:, :mixer_width]
    glu_pair = front[:, mixer_width : mixer_width + 2 * channels]
    step_at = mixer_width + 2 * channels
    step_values = front[:, step_at : step_at + head_count]
    short_rim = filter_input.shape[0] - 1
    long_rim = depth_filter.shape[0] - 1
    mixed = jax.nn.silu(
        causal_filter(
            passed_along(mixer_rows[row_count - short_rim :], "sp", 1),
            mixer_rows,
            jnp.concatenate([filter_input, filter_write, filter_read], axis=1),
        )
    ).astype(jnp.bfloat16)
    step_sizes = jax.nn.softplus(step_values.astype(jnp.float32) + step_bias)
    log_rates = -step_sizes * jnp.exp(rate_log) + decay_shift[0].T
    block_count = row_count // BLOCK
    blocked = jnp.cumsum(log_rates.reshape(block_count, BLOCK, head_count), axis=1)
    block_ends = blocked[:, -1]
    before = jnp.cumsum(block_ends, axis=0) - block_ends
    total_decay = before[-1] + block_ends[-1]
    to_end = jnp.exp(block_ends[:, None] - blocked).reshape(row_count, head_count) * step_sizes
    leading = jnp.exp(blocked + before[:, None]).reshape(row_count, head_count)
    blocked = blocked.reshape(row_count, head_count)

    def as_columns(array):
        return array.reshape(row_count, group_count, per_group).transpose(1, 0, 2)

    def as_rows(array):
        return array.T.reshape(group_count, per_group, row_count)

    wide = pl.BlockSpec((row_count, group_width), lambda g: (0, g))
    write_at, read_at = (width // STATE, width // STATE + group_count)
    write_spec = pl.BlockSpec((row_count, STATE), lambda g: (0, write_at + g))
    read_spec = pl.BlockSpec((row_count, STATE), lambda g: (0, read_at + g))
    column_spec = pl.BlockSpec((1, row_count, per_group), lambda g: (g, 0, 0))
    row_spec = pl.BlockSpec((1, per_group, row_count), lambda g: (g, 0, 0))
    state_spec = pl.BlockSpec((STATE, group_width), lambda g: (0, g))
    line_spec = pl.BlockSpec((1, group_width), lambda g: (0, g))
    local_rows, local_state = pl.pallas_call(
        local_kernel,
        grid=(group_count,),
        in_specs=[wide, write_spec, read_spec, column_spec, column_spec, row_spec, row_spec],
        out_specs=[wide, state_spec],
        out_shape=[
            jax.ShapeDtypeStruct((row_count, width), jnp.float32),
            jax.ShapeDtypeStruct((STATE, width), jnp.float32),
        ],
        cost_estimate=pl.CostEstimate(
            flops=8 * row_count * width * BLOCK, bytes_accessed=8 * row_count * width, transcendentals=0
        ),
    )(
        mixed,
        mixed,
        mixed,
        as_columns(blocked),
        as_columns(to_end),
        as_rows(blocked),
        as_rows(step_sizes),
    )
    decay_line = jnp.repeat(total_decay, HEAD_DIM)[None]
    decay_high = decay_line.astype(jnp.bfloat16)
    decay_low = (decay_line - decay_high.astype(jnp.float32)).astype(jnp.bfloat16)
    payload = jnp.concatenate(
        [
            local_state.astype(jnp.bfloat16),
            decay_high,
            decay_low,
            jnp.zeros((14, width), jnp.bfloat16),
        ],
        axis=0,
    )
    entering, reach = (jnp.zeros((STATE, width), jnp.float32), jnp.zeros((1, width), jnp.float32))
    for distance in range(1, length):
        earlier = passed_along(payload, "sp", distance).astype(jnp.float32)
        entering = entering + jnp.exp(reach) * earlier[:STATE]
        reach = reach + earlier[STATE : STATE + 1] + earlier[STATE + 1 : STATE + 2]
    opening = opening_state[0].reshape(width, STATE).T
    entering = entering + jnp.exp(reach) * opening
    state_out = pl.pallas_call(
        finish_kernel,
        grid=(group_count,),
        in_specs=[wide, wide, read_spec, wide, state_spec, column_spec, line_spec, line_spec],
        out_specs=wide,
        out_shape=jax.ShapeDtypeStruct((row_count, width), jnp.bfloat16),
        cost_estimate=pl.CostEstimate(
            flops=2 * row_count * width * STATE, bytes_accessed=10 * row_count * width, transcendentals=0
        ),
    )(
        local_rows,
        mixed,
        mixed,
        gate_values,
        entering,
        as_columns(leading),
        jnp.repeat(skip_gain, HEAD_DIM)[None],
        output_gain[None],
    )
    glu_rows = (
        glu_pair[:, :channels].astype(jnp.float32)
        * jax.nn.sigmoid(glu_pair[:, channels:].astype(jnp.float32))
    ).astype(jnp.bfloat16)
    filtered = causal_filter(
        passed_along(glu_rows[row_count - long_rim :], "sp", 1), glu_rows, depth_filter
    )
    channel_sums = lax.psum((jnp.sum(filtered, axis=1), jnp.sum(filtered * filtered, axis=1)), "tp")
    mean_value = channel_sums[0] / CM
    mean_square = channel_sums[1] / CM
    variance = mean_square - mean_value * mean_value
    normal_rows = (
        (filtered - mean_value[:, None]) * lax.rsqrt(variance + 1e-05)[:, None] * channel_gain
    )
    filter_out = jax.nn.silu(normal_rows).astype(jnp.bfloat16)
    share = lax.axis_size("fs")
    piece_rows = unproject_state.shape[0] // share
    first = lax.axis_index("fs") * piece_rows
    piece = jnp.concatenate(
        [
            lax.dynamic_slice_in_dim(unproject_state, first, piece_rows, 0),
            lax.dynamic_slice_in_dim(unproject_filter, first, piece_rows, 0),
        ],
        axis=0,
    )
    output_maps = lax.all_gather(piece, ("sp", "fs"), axis=0, tiled=True)
    output_maps = output_maps.reshape(length, share * 2 * piece_rows, piece.shape[1])
    joined = jnp.concatenate(
        [
            part[:, i * piece_rows : (i + 1) * piece_rows]
            for i in range(share)
            for part in (state_out, filter_out)
        ],
        axis=1,
    )
    partial_rows = jnp.concatenate(
        [
            jnp.dot(joined, output_maps[i], preferred_element_type=jnp.float32).astype(jnp.bfloat16)
            for i in range(length)
        ],
        axis=1,
    )
    summed = lax.psum_scatter(partial_rows, "tp", scatter_dimension=0, tiled=True)
    return summed[None]


def solution(mesh):
    in_specs = (
        P("fs", "sp", None),
        P(),
        P("sp", "tp"),
        P("sp", "tp"),
        P("sp", "tp"),
        P("sp", "tp"),
        P("sp", "tp"),
        P("sp", "tp"),
        P("sp", "tp"),
        P(None, "tp"),
        P(None, "tp"),
        P(None, "tp"),
        P("tp"),
        P("tp"),
        P("tp"),
        P("tp"),
        P("fs", "tp", None, None),
        P("fs", "tp", "sp"),
        P(None, "tp"),
        P("tp"),
        P("tp", "sp"),
        P("tp", "sp"),
    )
    out_specs = P("fs", ("sp", "tp"), None)
    return jax.shard_map(
        per_device, mesh=mesh, in_specs=in_specs, out_specs=out_specs, check_vma=False
    )
```
